256 devices in a mesh: sp: 32 (over z, x), fs: 4 (over y), tp: 2 (over core).
Axes of the slice: x: 4, y: 4, z: 8, core: 2. Of those that a mesh axis runs over, the one named last changes fastest.
Arguments:
- tokens: bfloat16 [4, 4096, 2048], P('fs', 'sp', 'tp'), may hold values from -6 to 6
- norm_gain: float32 [2048], replicated, may hold values from 0.1 to 1.9
- conv_gate_out: bfloat16 [2048, 512], P(('sp', 'fs'), 'tp'), may hold values from -0.125 to 0.125
- conv_gate_in: bfloat16 [2048, 512], P(('sp', 'fs'), 'tp'), may hold values from -0.125 to 0.125
- conv_value: bfloat16 [2048, 512], P(('sp', 'fs'), 'tp'), may hold values from -0.125 to 0.125
- conv_taps: float32 [3, 512], P(None, 'tp'), may hold values from -3.5 to 3.5
- recv_weight: bfloat16 [2048, 512], P(('sp', 'fs'), 'tp'), may hold values from -0.125 to 0.125
- key_weight: bfloat16 [2048, 512], P(('sp', 'fs'), 'tp'), may hold values from -0.125 to 0.125
- value_weight: bfloat16 [2048, 512], P(('sp', 'fs'), 'tp'), may hold values from -0.125 to 0.125
- decay_base: float32 [512], P('tp'), may hold values from -12.5 to -3.3
- decay_down: bfloat16 [2048, 64], replicated, may hold values from -0.125 to 0.125
- decay_up: bfloat16 [64, 512], P(None, 'tp'), may hold values from -1.5 to 1.5
- decay_shift: float32 [4, 4096, 8], P('fs', 'sp', 'tp'), may hold values from -0.7 to 11.5
- rate_base: float32 [512], P('tp'), may hold values from -4 to 4
- rate_down: bfloat16 [2048, 64], replicated, may hold values from -0.125 to 0.125
- rate_up: bfloat16 [64, 512], P(None, 'tp'), may hold values from -0.75 to 0.75
- head_gain: float32 [512], P('tp'), may hold values from 0.1 to 1.9
- out_conv: bfloat16 [512, 2048], P('tp', ('sp', 'fs')), may hold values from -0.1875 to 0.1875
- out_state: bfloat16 [512, 2048], P('tp', ('sp', 'fs')), may hold values from -0.1875 to 0.1875
Outputs:
- mixed_out: bfloat16 [4, 4096, 2048], P('fs', ('sp', 'tp'))
The draws below stay inside these ranges and needn't reach their ends.
All inputs are finite; a program needn't handle non-finite values.
Results may differ from the reference program's by a relative error of at most 0.015.
Values may be sent and summed in bfloat16 or wider, within the bound.
A program may use at most 64 MiB of HBM per device.

```python
import jax
import jax.numpy as jnp
from jax import lax

D = 2048
CW = 512
RH = 8
HD = 64
LOW = 64
TOK_DEV = 128
RW = 512
SEQS = 4
SEQ = 4096
N_TP = 2


def draw_decay_base(key, part):
    choose_key = jax.random.fold_in(key, 11)
    slow_key = jax.random.fold_in(key, 12)
    fast_key = jax.random.fold_in(key, 13)
    slow_share = 0.5
    slow_heads = jax.random.uniform(choose_key, (RH, 1), jnp.float32) < slow_share
    slow_values = jax.random.uniform(slow_key, (RH, HD), jnp.float32, -12.5, -10.5)
    fast_values = jax.random.uniform(fast_key, (RH, HD), jnp.float32, -4.3, -3.3)
    return jnp.where(slow_heads, slow_values, fast_values).reshape(RH * HD)


def draw_decay_shift(key, part):
    level_key = jax.random.fold_in(key, 21)
    spot_key = jax.random.fold_in(key, 22)
    lift_key = jax.random.fold_in(key, 23)
    blocks = SEQ // TOK_DEV
    level = jax.random.uniform(level_key, (SEQS, blocks, 1, RH), jnp.float32, -0.7, 0.7)
    level = jnp.broadcast_to(level, (SEQS, blocks, TOK_DEV, RH)).reshape(SEQS, SEQ, RH)
    spots = jax.random.randint(spot_key, (SEQS, 3), 0, SEQ)
    positions = jnp.arange(SEQ, dtype=jnp.int32)
    struck = jnp.any(positions[None, :, None] == spots[:, None, :], axis=-1)
    lift = jax.random.uniform(lift_key, (SEQS, SEQ, RH), jnp.float32, 10.5, 11.5)
    return jnp.where(struck[:, :, None], lift, level)


def block_scale(key, dims, cuts, least, high):
    loudness = 1.0
    for position, shards_of in cuts:
        heights = jax.random.uniform(jax.random.fold_in(jax.random.fold_in(key, 6), position), (shards_of,), jnp.float32, least / len(cuts), high / len(cuts))
        loudness = loudness * jnp.repeat(jnp.exp(heights), dims[position] // shards_of).reshape((-1,) + (1,) * (len(dims) - 1 - position))
    return loudness


def normal_values(own_key, shape, spread, bound, cuts=(), held_as=jnp.bfloat16):
    drawn = spread * jax.random.normal(own_key, shape, jnp.float32)
    if cuts:
        drawn = drawn * block_scale(own_key, shape, cuts, -0.22, 0.18)
    return jnp.clip(drawn, -bound, bound).astype(held_as)


def setup_inputs(seed: int = 0) -> dict:
    key_of = jax.random.split(jax.random.key(seed), 20)
    return {
        "tokens": normal_values(key_of[0], (SEQS, SEQ, D), 1.0, 6.0, ((0, 4), (1, 32), (2, 2))),
        "norm_gain": jnp.clip(1.0 + 0.18 * jax.random.normal(key_of[1], (D,), jnp.float32), 0.1, 1.9),
        "conv_gate_out": normal_values(key_of[2], (D, CW), D ** -0.5, 0.125, ((0, 128), (1, 2))),
        "conv_gate_in": normal_values(key_of[3], (D, CW), D ** -0.5, 0.125, ((0, 128), (1, 2))),
        "conv_value": normal_values(key_of[4], (D, CW), D ** -0.5, 0.125, ((0, 128), (1, 2))),
        "conv_taps": normal_values(key_of[5], (3, CW), 3 ** -0.5, 3.5, ((1, 2),), jnp.float32),
        "recv_weight": normal_values(key_of[6], (D, RW), D ** -0.5, 0.125, ((0, 128), (1, 2))),
        "key_weight": normal_values(key_of[7], (D, RW), D ** -0.5, 0.125, ((0, 128), (1, 2))),
        "value_weight": normal_values(key_of[8], (D, RW), D ** -0.5, 0.125, ((0, 128), (1, 2))),
        "decay_base": draw_decay_base(jax.random.fold_in(key_of[19], 71), 0),
        "decay_down": normal_values(key_of[10], (D, LOW), D ** -0.5, 0.125),
        "decay_up": normal_values(key_of[11], (LOW, RW), (LOW // 4) ** -0.5, 1.5, ((1, 2),)),
        "decay_shift": draw_decay_shift(jax.random.fold_in(key_of[19], 71), 0),
        "rate_base": normal_values(key_of[13], (RW,), 1.0, 4.0, ((0, 2),), jnp.float32),
        "rate_down": normal_values(key_of[14], (D, LOW), D ** -0.5, 0.125),
        "rate_up": normal_values(key_of[15], (LOW, RW), LOW ** -0.5, 0.75, ((1, 2),)),
        "head_gain": jnp.clip(1.0 + 0.18 * jax.random.normal(key_of[16], (RW,), jnp.float32), 0.1, 1.9),
        "out_conv": normal_values(key_of[17], (CW, D), (CW + RW) ** -0.5, 0.1875, ((0, 2), (1, 128))),
        "out_state": normal_values(key_of[18], (RW, D), (CW + RW) ** -0.5, 0.1875, ((0, 2), (1, 128))),
    }


RMS_EPS = 1e-05
GROUP_EPS = 0.00064
UNIT_EPS = 1e-06
HIGHEST = lax.Precision.HIGHEST

def project(normed, weight):
    return jnp.dot(normed, weight, preferred_element_type=jnp.float32).astype(jnp.bfloat16)

def recur(carried, inputs):
    keys_t, vals_t, recv_t, rate_t, decay_t = inputs
    keys_f = keys_t.astype(jnp.float32)
    vals_f = vals_t.astype(jnp.float32)
    recv_f = recv_t.astype(jnp.float32)
    unit_keys = keys_f * lax.rsqrt(lax.optimization_barrier(jnp.sum(keys_f * keys_f, axis=-1, keepdims=True)) + UNIT_EPS)
    removed = jnp.einsum('shvk,shk->shv', carried, -unit_keys, precision=HIGHEST)
    carried = carried * jnp.exp(decay_t)[:, :, None, :] + removed[..., None] * (unit_keys * rate_t)[:, :, None, :] + vals_f[..., None] * (keys_f * rate_t)[:, :, None, :]
    return (carried, jnp.einsum('shvk,shk->shv', carried, recv_f, precision=HIGHEST))

def reference(tokens, norm_gain, conv_gate_out, conv_gate_in, conv_value, conv_taps, recv_weight, key_weight, value_weight, decay_base, decay_down, decay_up, decay_shift, rate_base, rate_down, rate_up, head_gain, out_conv, out_state):
    rows_all = SEQS * SEQ
    flat = tokens.reshape(rows_all, D).astype(jnp.float32)
    normed = (flat * lax.rsqrt(lax.optimization_barrier(jnp.mean(flat * flat, axis=-1, keepdims=True)) + RMS_EPS) * norm_gain).astype(jnp.bfloat16)
    gate_out = project(normed, conv_gate_out).astype(jnp.float32).reshape(SEQS, SEQ, CW)
    gate_in = project(normed, conv_gate_in).astype(jnp.float32)
    conv_in = project(normed, conv_value).astype(jnp.float32)
    mixed_in = (gate_in * conv_in).reshape(SEQS, SEQ, CW)
    padded = jnp.pad(mixed_in, ((0, 0), (2, 0), (0, 0)))
    convolved = padded[:, 0:SEQ] * conv_taps[0] + padded[:, 1:SEQ + 1] * conv_taps[1] + padded[:, 2:SEQ + 2] * conv_taps[2]
    conv_out = (gate_out * convolved).astype(jnp.bfloat16).reshape(rows_all, CW)
    recv = project(normed, recv_weight)
    keys = project(normed, key_weight)
    vals = project(normed, value_weight)
    decay_low = jnp.tanh(jnp.dot(normed, decay_down, preferred_element_type=jnp.float32)).astype(jnp.bfloat16)
    rate_low = project(normed, rate_down)
    decay_pre = decay_base + jnp.dot(decay_low, decay_up, preferred_element_type=jnp.float32)
    log_base = -jax.nn.softplus(-decay_pre) - 0.5
    log_decay = -jnp.exp(log_base.reshape(SEQS, SEQ, RH, HD) + decay_shift[..., None])
    learn_rate = jax.nn.sigmoid(rate_base + jnp.dot(rate_low, rate_up, preferred_element_type=jnp.float32))

    def by_time(field):
        return jnp.swapaxes(field.reshape(SEQS, SEQ, RH, HD), 0, 1)
    start_state = jnp.zeros((SEQS, RH, HD, HD), jnp.float32)
    final_state, read_out = lax.scan(recur, start_state, (by_time(keys), by_time(vals), by_time(recv), by_time(learn_rate), by_time(log_decay)))
    state_read = jnp.swapaxes(read_out, 0, 1)
    centre = lax.optimization_barrier(jnp.mean(state_read, axis=-1, keepdims=True))
    centred = state_read - centre
    variance = lax.optimization_barrier(jnp.mean(centred * centred, axis=-1, keepdims=True))
    state_out = ((centred * lax.rsqrt(variance + GROUP_EPS)).reshape(rows_all, RW) * head_gain).astype(jnp.bfloat16)
    conv_block = CW // N_TP
    state_block = RW // N_TP
    total = jnp.zeros((rows_all, D), jnp.float32)
    for group in range(N_TP):
        partial_sum = jnp.dot(conv_out[:, group * conv_block:(group + 1) * conv_block], out_conv[group * conv_block:(group + 1) * conv_block], preferred_element_type=jnp.float32) + jnp.dot(state_out[:, group * state_block:(group + 1) * state_block], out_state[group * state_block:(group + 1) * state_block], preferred_element_type=jnp.float32)
        rounded = lax.optimization_barrier(partial_sum.astype(jnp.bfloat16))
        total = total + rounded.astype(jnp.float32)
    return total.astype(jnp.bfloat16).reshape(SEQS, SEQ, D)
```

```python
import functools

import jax
import jax.numpy as jnp
from jax import lax
from jax.experimental import pallas as pl
from jax.experimental.pallas import tpu as pltpu
from jax.sharding import Mesh
from jax.sharding import PartitionSpec as P

SP = ("sp_0", "sp_1")
SP_FS = ("sp_0", "sp_1", "fs")
SP_TP = ("sp_0", "sp_1", "tp")
BF = jnp.bfloat16
F32 = jnp.float32
RMS_EPS = 1e-05
GROUP_EPS = 0.00064
UNIT_EPS = 1e-06
T = 128
HD = 64
NZ, NX, NY = 8, 4, 4
MESH = pl.DeviceIdType.MESH
VM = pltpu.VMEM


def at_axis(name, index):
    return {name: index}


class Copies:
    def __init__(self, send_sems, recv_sems):
        self.send_sems, self.recv_sems = send_sems, recv_sems
        self.used = 0
        self.sent = []

    def slot(self):
        self.used += 1
        return self.used - 1

    def make(self, slot, src, dst, where):
        return pltpu.make_async_remote_copy(
            src_ref=src,
            dst_ref=dst,
            send_sem=self.send_sems.at[slot],
            recv_sem=self.recv_sems.at[slot],
            device_id=where,
            device_id_type=MESH,
        )

    def send(self, slot, src, dst, where):
        copy = self.make(slot, src, dst, where)
        copy.start()
        self.sent.append(copy)

    def arrived(self, slot, ref, where):
        self.make(slot, ref, ref, where).wait_recv()

    def finish(self):
        for copy in self.sent:
            copy.wait_send()


def gather_kernel(
    tok, wsl, own, shift, tok_all, w_all, o_slab, sh_all, w_own, local_sems, send_sems, recv_sems
):
    z, x = lax.axis_index("sp_0"), lax.axis_index("sp_1")
    y, c = lax.axis_index("fs"), lax.axis_index("tp")

    def up(i, by, n):
        return lax.rem(i + by + n, n)

    locals_ = [
        pltpu.make_async_copy(tok, tok_all.at[x, c], local_sems.at[0]),
        pltpu.make_async_copy(wsl, w_own, local_sems.at[1]),
        pltpu.make_async_copy(wsl.at[x], w_all.at[z, x, y], local_sems.at[2]),
        pltpu.make_async_copy(own, o_slab.at[z, y], local_sems.at[3]),
        pltpu.make_async_copy(shift, sh_all.at[x], local_sems.at[4]),
    ]
    for copy in locals_:
        copy.start()
    barrier = pltpu.get_barrier_semaphore()
    peers = [at_axis("sp_1", up(x, d, NX)) for d in (1, 2, 3)]
    peers += [at_axis("fs", up(y, d, NY)) for d in (1, 2, 3)]
    peers += [at_axis("sp_0", up(z, 1, NZ)), at_axis("sp_0", up(z, -1, NZ))]
    peers += [at_axis("tp", 1 - c)]
    for peer in peers:
        pl.semaphore_signal(barrier, inc=1, device_id=peer, device_id_type=MESH)
    pl.semaphore_wait(barrier, len(peers))
    for copy in locals_:
        copy.wait()

    net = Copies(send_sems, recv_sems)
    todo = []
    right, left = at_axis("sp_1", up(x, 1, NX)), at_axis("sp_1", up(x, -1, NX))
    partner = at_axis("tp", 1 - c)

    in_slots = [None] + [net.slot() for _ in range(3)]
    sh_slots = [None] + [net.slot() for _ in range(3)]
    for d in (1, 2, 3):
        to = up(x, d, NX)
        net.send(in_slots[d], w_own.at[to], w_all.at[z, x, y], at_axis("sp_1", to))
    for d in (1, 2, 3):
        net.send(sh_slots[d], sh_all.at[x], sh_all.at[x], at_axis("sp_1", up(x, d, NX)))

    zr, zl = at_axis("sp_0", up(z, 1, NZ)), at_axis("sp_0", up(z, -1, NZ))

    def z_ring(view, parts, ready, start, step):
        slots = {}
        half = parts // 2
        for k in range(1, 5):
            for way in (1, -1):
                for e in range(parts):
                    if k < 4 or (e < half) == (way == 1):
                        slots[way, k, e] = net.slot()
        for k in range(1, 5):
            for e in range(parts):

                def act(k=k, e=e):
                    if k == 1:
                        ready(e)
                    for way, nxt in ((1, zr), (-1, zl)):
                        ref = view(up(z, way * (1 - k), NZ), e)
                        if k > 1:
                            net.arrived(slots[way, k - 1, e], ref, nxt)
                        if (way, k, e) in slots:
                            net.send(slots[way, k, e], ref, ref, nxt)

                todo.append((start + step * (k - 1) + 0.01 * e, act))

        def last():
            for way, nxt in ((1, zr), (-1, zl)):
                for e in range(parts):
                    if (way, 4, e) in slots:
                        net.arrived(slots[way, 4, e], view(up(z, -4, NZ), e), nxt)

        todo.append((start + step * 4, last))

    z_ring(lambda i, e: o_slab.at[i, y, pl.ds(8 * e, 8)], 2, lambda e: None, 0.5, 2.2)

    yr, yl = at_axis("fs", up(y, 1, NY)), at_axis("fs", up(y, -1, NY))
    y_slots = {(way, k, h): net.slot() for way in (1, -1) for k in (1, 2) for h in (0, 1)
               if k == 1 or (h == 0) == (way == 1)}

    def o_view(i, h):
        return o_slab.at[pl.ds(4 * h, 4), i]

    def o_first():
        for way, nxt in ((1, yr), (-1, yl)):
            for h in (0, 1) if way == 1 else (1, 0):
                net.send(y_slots[way, 1, h], o_view(y, h), o_view(y, h), nxt)

    def o_second():
        for way, nxt in ((1, yr), (-1, yl)):
            h = 0 if way == 1 else 1
            ref = o_view(up(y, -way, NY), h)
            net.arrived(y_slots[way, 1, h], ref, nxt)
            net.send(y_slots[way, 2, h], ref, ref, nxt)

    def o_last():
        for way, nxt in ((1, yr), (-1, yl)):
            h = 0 if way == 1 else 1
            ref = o_view(up(y, -way, NY), 1 - h)
            net.arrived(y_slots[way, 1, 1 - h], ref, nxt)
            ref = o_view(up(y, 2, NY), h)
            net.arrived(y_slots[way, 2, h], ref, nxt)

    todo += [(9.4, o_first), (13.0, o_second), (17.0, o_last)]

    tok_slots = {(way, k, h): net.slot() for way in (1, -1) for k in (1, 2) for h in (0, 1)
                 if k == 1 or (h == 0) == (way == 1)}
    chip_slots = {(d, h): net.slot() for d in range(4) for h in (0, 1)}

    def t_view(i, h, core=None):
        return tok_all.at[i, c if core is None else core, pl.ds(64 * h, 64)]

    def across(d, h):
        ref = t_view(up(x, d, NX), h)
        net.send(chip_slots[d, h], ref, ref, partner)

    def t_first():
        for h in (0, 1):
            for way, nxt in ((1, right), (-1, left)):
                g = h if way == 1 else 1 - h
                net.send(tok_slots[way, 1, g], t_view(x, g), t_view(x, g), nxt)
        for h in (0, 1):
            across(0, h)

    def t_second():
        for way, nxt in ((1, right), (-1, left)):
            h = 0 if way == 1 else 1
            ref = t_view(up(x, -way, NX), h)
            net.arrived(tok_slots[way, 1, h], ref, nxt)
            net.send(tok_slots[way, 2, h], ref, ref, nxt)
            across((4 - way) % 4, h)

    def t_third():
        for way, nxt in ((1, right), (-1, left)):
            h = 1 if way == 1 else 0
            net.arrived(tok_slots[way, 1, h], t_view(up(x, -way, NX), h), nxt)
            across((4 - way) % 4, h)

    def t_fourth():
        for way, nxt in ((1, right), (-1, left)):
            h = 0 if way == 1 else 1
            net.arrived(tok_slots[way, 2, h], t_view(up(x, 2, NX), h), nxt)
            across(2, h)

    def t_last():
        for d in range(4):
            for h in (0, 1):
                net.arrived(chip_slots[d, h], t_view(up(x, d, NX), h, 1 - c), partner)
        for d in (1, 2, 3):
            net.arrived(sh_slots[d], sh_all.at[up(x, -d, NX)], at_axis("sp_1", up(x, d, NX)))

    todo += [(0.0, t_first), (4.6, t_second), (7.5, t_third), (11.0, t_fourth), (20.0, t_last)]

    yp_slots = {(e, d): net.slot() for e in (1, 2, 3) for d in range(4)}

    def w_piece(d):
        def act():
            xi = up(x, -d, NX)
            ref = w_all.at[z, xi, y]
            if d:
                net.arrived(in_slots[d], ref, at_axis("sp_1", xi))
            for e in (1, 2, 3):
                net.send(yp_slots[e, d], ref, ref, at_axis("fs", up(y, e, NY)))

        return act

    todo += [(0.1, w_piece(0)), (2.0, w_piece(1)), (2.1, w_piece(3)), (2.2, w_piece(2))]

    def w_ready(e):
        if e:
            for d in range(4):
                net.arrived(
                    yp_slots[e, d], w_all.at[z, up(x, -d, NX), up(y, -e, NY)], at_axis("fs", up(y, -e, NY))
                )

    z_ring(lambda i, e: w_all.at[i, :, up(y, -e, NY)], 4, w_ready, 2.4, 4.5)

    for _, act in sorted(todo, key=lambda item: item[0]):
        act()
    net.finish()


N_GATHER = 200


def gather(tok, wsl, own, shift):
    sds = jax.ShapeDtypeStruct
    hbm = pl.BlockSpec(memory_space=pltpu.HBM)
    vmem = pl.BlockSpec(memory_space=VM)
    return pl.pallas_call(
        gather_kernel,
        out_shape=(
            sds((NX, 2, T, 1024), BF),
            sds((NZ, NX, NY, 16, 384), BF),
            sds((NZ, NY, 16, 512), BF),
            sds((NX, 4, T), F32),
        ),
        in_specs=[hbm] * 4,
        out_specs=(vmem,) * 4,
        scratch_shapes=[
            VM((NX, 16, 384), BF),
            pltpu.SemaphoreType.DMA((5,)),
            pltpu.SemaphoreType.DMA((N_GATHER,)),
            pltpu.SemaphoreType.DMA((N_GATHER,)),
        ],
        compiler_params=pltpu.CompilerParams(collective_id=1, has_side_effects=True),
        name="gather",
    )(tok, wsl, own, shift)


def dot(a, b, ca=1, cb=0):
    return lax.dot_general(a, b, (((ca,), (cb,)), ((), ())), preferred_element_type=F32)


def bdot(a, b, ca=1, cb=0):
    return dot(a.astype(BF), b.astype(BF), ca, cb)


def split3(v):
    hi = v.astype(BF)
    rest = v - hi.astype(F32)
    mid = rest.astype(BF)
    return hi, mid, (rest - mid.astype(F32)).astype(BF)


def iota2(shape):
    return lax.broadcasted_iota(jnp.int32, shape, 0), lax.broadcasted_iota(jnp.int32, shape, 1)


def level_masks():
    i, j = iota2((T, T))
    masks = []
    h = 1
    while h < T:
        mid = (i // (2 * h)) * (2 * h) + h
        masks.append(((i >= mid) & (j >= mid) & (j < i)) | ((i < mid) & (j > i) & (j < mid)))
        h *= 2
    return masks + [j < i, j > i]


def own_head(x, array):
    out = array[:, :HD]
    for h in range(1, NX):
        out = jnp.where(x == h, array[:, h * HD : (h + 1) * HD], out)
    return out


def unit_solve(X, u, w, a, b, k, r, v):
    lane = slice(u * HD, (u + 1) * HD)
    i, j = iota2((T, T))
    eye = i == j
    right = jnp.concatenate([b, k], 0)
    left = jnp.concatenate([a, r * w], 0)
    diag = bdot(r, right, 1, 1)
    arb = jnp.where(eye, diag[:, :T], 0.0)
    ark = jnp.where(eye, diag[:, T:], 0.0)
    aak = jnp.zeros((T, T), F32)
    inv = jnp.where(eye, 1.0, 0.0)
    h, level = 1, 0
    while h < T:
        x = X[level * T : (level + 1) * T, lane]
        xx = jnp.concatenate([x, x], 0)
        score = bdot(left * xx, right * xx, 1, 1)
        mask = ((i // (2 * h)) == (j // (2 * h))) & ((i // h) % 2 == 1) & ((j // h) % 2 == 0)
        aab = jnp.where(mask, score[:T, :T], 0.0)
        aak = jnp.where(mask, score[:T, T:], aak)
        arb = jnp.where(mask, score[T:, :T], arb)
        ark = jnp.where(mask, score[T:, T:], ark)
        inv = inv + (aab if h == 1 else bdot(inv, bdot(aab, inv)))
        h, level = 2 * h, level + 1
    before = X[7 * T : 8 * T, lane]
    after = X[8 * T : 9 * T, lane]
    a_start, r_start = a * before, r * w * before
    b_end, k_end = b * after, k * after
    w_all = before[T - 1 : T] * w[T - 1 : T]
    uz = bdot(inv, jnp.concatenate([a_start, bdot(aak, v)], 1))
    writes = jnp.concatenate([uz, jnp.concatenate([jnp.zeros_like(v), v], 1)], 0)
    reads = bdot(jnp.concatenate([arb, ark], 1), writes)
    reads = reads + jnp.concatenate([r_start, jnp.zeros_like(r)], 1)
    i, j = iota2((HD, 2 * HD))
    passed = bdot(jnp.concatenate([b_end, k_end], 0).T, writes)
    passed = passed + jnp.where(i == j, jnp.concatenate([w_all, w_all], 1), 0.0)
    return reads, passed


def local_kernel(
    tok_all, gain, w_all, dd, rd, sh_all, params, dup, rup, reads_out, passed_out, total_out, conv_out, normed
):
    x = lax.axis_index("sp_1")
    rows = NX * T
    for u in range(NX):
        t0, t1 = tok_all[u, 0].astype(F32), tok_all[u, 1].astype(F32)
        square = jnp.sum(t0 * t0, -1, keepdims=True) + jnp.sum(t1 * t1, -1, keepdims=True)
        scale = lax.rsqrt(square / 2048.0 + RMS_EPS)
        normed[u * T : (u + 1) * T, :1024] = (t0 * scale * gain[:, :1024]).astype(BF)
        normed[u * T : (u + 1) * T, 1024:] = (t1 * scale * gain[:, 1024:]).astype(BF)
    n = normed[...]
    main = dot(n, w_all[...]).astype(BF)
    low = dot(n, jnp.concatenate([dd[...], rd[...]], 1))
    conv_out[...] = jnp.concatenate(
        [main[:, HD : 2 * HD].astype(F32) * main[:, 2 * HD : 3 * HD].astype(F32), main[:, :HD].astype(F32)], 1
    )
    recv = main[:, 3 * HD : 4 * HD].astype(F32)
    keys = main[:, 4 * HD : 5 * HD].astype(F32)
    vals = main[:, 5 * HD :].astype(F32)
    decay_low = jnp.tanh(low[:, :HD]).astype(BF)
    rate_low = low[:, HD:].astype(BF)
    table = own_head(x, params[...])
    pre = table[0:1] + dot(decay_low, own_head(x, dup[...]))
    rate = jax.nn.sigmoid(table[1:2] + dot(rate_low, own_head(x, rup[...])))
    base = -(jnp.maximum(-pre, 0.0) + jnp.log1p(jnp.exp(-jnp.abs(pre)))) - 0.5
    i, j = iota2((T, T))
    eye = i == j
    logs = []
    for u in range(NX):
        row = sh_all[u]
        mine = row[0:1]
        for h in range(1, NX):
            mine = jnp.where(x == h, row[h : h + 1], mine)
        column = jnp.sum(jnp.where(eye, mine, 0.0), -1, keepdims=True)
        logs.append(-jnp.exp(base[u * T : (u + 1) * T] + column))
    unit = keys * lax.rsqrt(jnp.sum(keys * keys, -1, keepdims=True) + UNIT_EPS)
    masks = jnp.concatenate([jnp.where(m, 1.0, 0.0) for m in level_masks()], 0).astype(BF)
    sums = sum(dot(masks, part) for part in split3(jnp.concatenate(logs, 1)))
    X = jnp.exp(sums)
    total = None
    i, j = iota2((HD, 2 * HD))
    for u in range(NX):
        s = slice(u * T, (u + 1) * T)
        reads, passed = unit_solve(
            X, u, jnp.exp(logs[u]), -unit[s], unit[s] * rate[s], keys[s] * rate[s], recv[s], vals[s]
        )
        reads_out[u] = reads
        passed_out[u] = passed
        if total is None:
            total = passed
        else:
            total = bdot(passed[:, :HD], total) + jnp.where(j >= HD, passed, 0.0)
    total_out[...] = total.astype(BF)


def local(tok_all, gain, w_all, dd, rd, sh_all, params, dup, rup):
    sds = jax.ShapeDtypeStruct
    vmem = pl.BlockSpec(memory_space=VM)
    return pl.pallas_call(
        local_kernel,
        out_shape=(
            sds((NX, T, 2 * HD), F32),
            sds((NX, HD, 2 * HD), F32),
            sds((HD, 2 * HD), BF),
            sds((NX * T, 2 * HD), F32),
        ),
        in_specs=[vmem] * 9,
        out_specs=(vmem,) * 4,
        scratch_shapes=[VM((NX * T, 2048), BF)],
        name="local",
    )(tok_all, gain, w_all, dd, rd, sh_all, params, dup, rup)


def finish_kernel(
    o_slab, reads, passed, total, conv, params, out,
    o_all, prefix, halo, state, pack, heads, to_partner, from_partner, own_part,
    local_sems, send_sems, recv_sems,
):
    z, x = lax.axis_index("sp_0"), lax.axis_index("sp_1")
    c = lax.axis_index("tp")

    def up(i, by, n):
        return lax.rem(i + by + n, n)

    mine = pltpu.make_async_copy(o_slab, o_all.at[:, x], local_sems.at[0])
    mine.start()
    barrier = pltpu.get_barrier_semaphore()
    peers = [at_axis("sp_1", up(x, d, NX)) for d in (1, 2, 3)]
    peers += [at_axis("sp_0", up(z, d, NZ)) for d in range(1, NZ)]
    peers += [at_axis("tp", 1 - c)]
    for peer in peers:
        pl.semaphore_signal(barrier, inc=1, device_id=peer, device_id_type=MESH)
    pl.semaphore_wait(barrier, len(peers))

    net = Copies(send_sems, recv_sems)
    net.used = 2 * NZ
    halo_slot = net.slot()
    send_slots = [net.slot() for _ in range(NZ)]

    def total_copy(to, d):
        return pltpu.make_async_remote_copy(
            src_ref=total, dst_ref=prefix.at[z], send_sem=send_sems.at[send_slots[d]],
            recv_sem=recv_sems.at[z], device_id=at_axis("sp_0", to), device_id_type=MESH,
        )

    for d in range(NZ - 1, 0, -1):

        @pl.when(z + d < NZ)
        def _(d=d):
            total_copy(lax.rem(z + d, NZ), d).start()

    tail = conv.at[pl.ds(NX * T - 8, 8)]

    @pl.when(z + 1 < NZ)
    def _():
        net.make(halo_slot, tail, halo, at_axis("sp_0", up(z, 1, NZ))).start()

    mine.wait()
    right, left = at_axis("sp_1", up(x, 1, NX)), at_axis("sp_1", up(x, -1, NX))
    slots = {(way, k, h): net.slot() for way in (1, -1) for k in (1, 2) for h in (0, 1)
             if k == 1 or (h == 0) == (way == 1)}

    def o_view(i, h):
        return o_all.at[pl.ds(4 * h, 4), i]

    for h in (0, 1):
        for way, nxt in ((1, right), (-1, left)):
            g = h if way == 1 else 1 - h
            net.send(slots[way, 1, g], o_view(x, g), o_view(x, g), nxt)

    table = own_head(x, params[...])

    @pl.when(z == 0)
    def _():
        halo[...] = jnp.zeros_like(halo)

    @pl.when(z > 0)
    def _():
        net.arrived(halo_slot, halo, at_axis("sp_0", up(z, -1, NZ)))

    for u in range(NX):
        s = slice(u * T, (u + 1) * T)
        before = halo[...] if u == 0 else conv[u * T - 8 : u * T]
        ext = jnp.concatenate([before, conv[s]], 0)[:, :HD]
        mixed = ext[6 : 6 + T] * table[3:4] + ext[7 : 7 + T] * table[4:5] + ext[8 : 8 + T] * table[5:6]
        pack[u, :, :HD] = (conv[s][:, HD:] * mixed).astype(BF)

    state[...] = jnp.zeros_like(state)
    for zz in range(NZ - 1):

        @pl.when(zz < z)
        def _(zz=zz):
            pltpu.make_async_remote_copy(
                src_ref=total, dst_ref=prefix.at[zz], send_sem=send_sems.at[0],
                recv_sem=recv_sems.at[zz], device_id=at_axis("sp_0", up(z, 1, NZ)), device_id_type=MESH,
            ).wait_recv()
            step = prefix[zz]
            state[...] = bdot(step[:, :HD], state[...]) + step[:, HD:].astype(F32)

    entering = state[...]
    for u in range(NX):
        got = reads[u]
        read = got[:, HD:] + bdot(got[:, :HD], entering)
        if u < NX - 1:
            step = passed[u]
            entering = bdot(step[:, :HD], entering) + step[:, HD:]
        centred = read - jnp.mean(read, -1, keepdims=True)
        variance = jnp.mean(centred * centred, -1, keepdims=True)
        pack[u, :, HD:] = (centred * lax.rsqrt(variance + GROUP_EPS) * table[2:3]).astype(BF)

    for way, nxt in ((1, right), (-1, left)):
        h = 0 if way == 1 else 1
        ref = o_view(up(x, -way, NX), h)
        net.arrived(slots[way, 1, h], ref, nxt)
        net.send(slots[way, 2, h], ref, ref, nxt)

    head_slots = [None] + [net.slot() for _ in range(3)]
    for d in (1, 2, 3):
        to = up(x, d, NX)
        net.send(head_slots[d], pack.at[to], heads.at[x], at_axis("sp_1", to))
    heads[x] = pack[x]
    for d in (1, 2, 3):
        net.arrived(head_slots[d], heads.at[up(x, -d, NX)], at_axis("sp_1", up(x, d, NX)))
    for way, nxt in ((1, right), (-1, left)):
        h = 0 if way == 1 else 1
        net.arrived(slots[way, 1, 1 - h], o_view(up(x, -way, NX), 1 - h), nxt)
        net.arrived(slots[way, 2, h], o_view(up(x, 2, NX), h), nxt)

    theirs = pl.multiple_of((1 - c) * 64, 64)
    ours = pl.multiple_of(c * 64, 64)
    lhs = jnp.concatenate(
        [
            jnp.concatenate([heads[h, pl.ds(theirs, 64), :] for h in range(NX)], 1),
            jnp.concatenate([heads[h, pl.ds(ours, 64), :] for h in range(NX)], 1),
        ],
        0,
    )
    chip_slots = [net.slot() for _ in range(NZ)]
    partner = at_axis("tp", 1 - c)
    for zz in range(NZ):
        part = dot(lhs, o_all[zz].reshape(256, 512), 1, 1).astype(BF)
        to_partner[zz] = part[:64]
        own_part[zz] = part[64:]
        net.send(chip_slots[zz], to_partner.at[zz], from_partner.at[zz], partner)
    for zz in range(NZ):
        net.arrived(chip_slots[zz], from_partner.at[zz], partner)
        out[:, zz * 256 : (zz + 1) * 256] = (
            own_part[zz].astype(F32) + from_partner[zz].astype(F32)
        ).astype(BF)
    net.finish()
    for d in range(NZ - 1, 0, -1):

        @pl.when(z + d < NZ)
        def _(d=d):
            total_copy(lax.rem(z + d, NZ), d).wait_send()

    @pl.when(z + 1 < NZ)
    def _():
        net.make(halo_slot, tail, halo, at_axis("sp_0", up(z, 1, NZ))).wait_send()


def finish(o_slab, reads, passed, total, conv, params):
    hbm = pl.BlockSpec(memory_space=pltpu.HBM)
    vmem = pl.BlockSpec(memory_space=VM)
    return pl.pallas_call(
        finish_kernel,
        out_shape=jax.ShapeDtypeStruct((64, 2048), BF),
        in_specs=[hbm] + [vmem] * 5,
        out_specs=vmem,
        scratch_shapes=[
            VM((NZ, NX, NY, 16, 512), BF),
            VM((NZ, HD, 2 * HD), BF),
            VM((8, 2 * HD), F32),
            VM((HD, HD), F32),
            VM((NX, T, 2 * HD), BF),
            VM((NX, T, 2 * HD), BF),
            VM((NZ, 64, 256), BF),
            VM((NZ, 64, 256), BF),
            VM((NZ, 64, 256), BF),
            pltpu.SemaphoreType.DMA((1,)),
            pltpu.SemaphoreType.DMA((64,)),
            pltpu.SemaphoreType.DMA((64,)),
        ],
        compiler_params=pltpu.CompilerParams(collective_id=2, has_side_effects=True),
        name="finish",
    )(o_slab, reads, passed, total, conv, params)


def body(
    tokens, norm_gain, conv_gate_out, conv_gate_in, conv_value, conv_taps, recv_weight, key_weight,
    value_weight, decay_base, decay_down, decay_up, decay_shift, rate_base, rate_down, rate_up,
    head_gain, out_conv, out_state,
):
    wsl = jnp.stack([conv_gate_out, conv_gate_in, conv_value, recv_weight, key_weight, value_weight], 1)
    wsl = wsl.reshape(16, 6, NX, HD).transpose(2, 0, 1, 3).reshape(NX, 16, 6 * HD)
    own = jnp.stack([out_conv.reshape(NX, HD, 16), out_state.reshape(NX, HD, 16)], 1)
    own = own.reshape(8 * HD, 16).T
    shift = decay_shift.reshape(T, NX).T
    params = jnp.concatenate(
        [decay_base[None], rate_base[None], head_gain[None], conv_taps, jnp.zeros((2, 256), F32)], 0
    )
    tok_all, w_all, o_slab, sh_all = gather(tokens.reshape(T, 1024), wsl, own, shift)
    reads, passed, total, conv = local(
        tok_all, norm_gain.reshape(1, 2048), w_all.reshape(2048, 384), decay_down, rate_down, sh_all,
        params, decay_up, rate_up,
    )
    return finish(o_slab, reads, passed, total, conv, params).reshape(1, 64, 2048)


def solution(mesh):
    torus = Mesh(
        mesh.devices.reshape(NZ, NX, mesh.shape["fs"], mesh.shape["tp"]), ("sp_0", "sp_1", "fs", "tp")
    )
    placed = (
        P("fs", SP, "tp"), P(), P(SP_FS, "tp"), P(SP_FS, "tp"), P(SP_FS, "tp"), P(None, "tp"),
        P(SP_FS, "tp"), P(SP_FS, "tp"), P(SP_FS, "tp"), P("tp"), P(), P(None, "tp"), P("fs", SP, "tp"),
        P("tp"), P(), P(None, "tp"), P("tp"), P("tp", SP_FS), P("tp", SP_FS),
    )
    return jax.shard_map(
        body, mesh=torus, in_specs=placed, out_specs=P("fs", SP_TP, None), check_vma=False
    )
```
